32 devices in a mesh: row: 4 (over y, x), col: 8 (over z, core).
Axes of the slice: x: 2, y: 2, z: 4, core: 2. Of those that a mesh axis runs over, the one named last changes fastest.
Arguments:
- tokens: bfloat16 [2, 2048, 1024], P(None, ('row', 'col')), may hold values from -6 to 6
- proj_weight: bfloat16 [1024, 256], replicated, may hold values from -0.1875 to 0.1875
- gate_weight: bfloat16 [1024, 256], replicated, may hold values from -0.1875 to 0.1875
- out_weight: bfloat16 [256, 1024], replicated, may hold values from -0.375 to 0.375
Outputs:
- mixed_out: bfloat16 [2, 2048, 1024], P(None, ('col', 'row'))
The draws below stay inside these ranges and needn't reach their ends.
All inputs are finite; a program needn't handle non-finite values.
Results may differ from the reference program's by a relative error of at most 0.02.
Values may be sent and summed in bfloat16 or wider, within the bound.
A program may use at most 64 MiB of HBM per device.

```python
import jax
import jax.numpy as jnp

SEQS = 2
D = 1024
GROUPS = 4
GROUP_DIM = 64
FW = 256
SEQ = 2048


def levels(key, shape, split, smallest, high):
    def one(axis_at, parts):
        heights = jax.random.uniform(jax.random.fold_in(jax.random.fold_in(key, 6), axis_at), (parts,), jnp.float32, smallest / len(split), high / len(split))
        return jnp.repeat(jnp.exp(heights), shape[axis_at] // parts).reshape((-1,) + (1,) * (len(shape) - axis_at - 1))

    factor_of = one(*split[0])
    for cut in split[1:]:
        factor_of = factor_of * one(*cut)
    return factor_of


def bell_draw(own_key, extent, spread, limit, pieces=(), kind=jnp.bfloat16):
    factor_of = levels(own_key, extent, pieces, -0.22, 0.18) if pieces else 1.0
    entries = jax.random.normal(own_key, extent, jnp.float32) * spread * factor_of
    return jnp.minimum(jnp.maximum(entries, -limit), limit).astype(kind)


def setup_inputs(seed: int = 0) -> dict:
    seeds = jax.random.split(jax.random.key(seed), 5)
    return {
        "tokens": bell_draw(seeds[0], (SEQS, SEQ, D), 1.0, 6.0, ((1, 32),)),
        "proj_weight": bell_draw(seeds[1], (D, FW), D ** -0.5, 0.1875),
        "gate_weight": bell_draw(seeds[2], (D, FW), D ** -0.5, 0.1875),
        "out_weight": bell_draw(seeds[3], (FW, D), FW ** -0.5, 0.375),
    }


def reference(tokens, proj_weight, gate_weight, out_weight):
    flattened = tokens.reshape(SEQS * SEQ, D)
    hidden = jnp.dot(flattened, proj_weight, preferred_element_type=jnp.float32).astype(jnp.bfloat16)
    gate_pre = jnp.dot(flattened, gate_weight, preferred_element_type=jnp.float32)
    mix_input = (hidden.astype(jnp.float32) * jax.nn.silu(gate_pre)).astype(jnp.bfloat16)
    grouped = mix_input.astype(jnp.float32).reshape(SEQS, SEQ, GROUPS, GROUP_DIM)
    spectrum = jnp.fft.fft2(grouped, axes=(1, 3), norm="ortho").real
    mixed = spectrum.astype(jnp.bfloat16).reshape(SEQS * SEQ, FW)
    result_out = jnp.dot(mixed, out_weight, preferred_element_type=jnp.float32).astype(jnp.bfloat16)
    return result_out.reshape(SEQS, SEQ, D)
```

```python
import functools
import math

import jax
import jax.numpy as jnp
import numpy as np
from jax import lax
from jax.experimental import pallas as pl
from jax.experimental.pallas import tpu as pltpu
from jax.sharding import PartitionSpec as P

GROUPS = 4
LANES = 128
MESH = pl.DeviceIdType.MESH


def tables(length, set_count, block, seq_count, chan):
    set_freqs = length // set_count
    half = block // 2
    per_tile = LANES // half
    kappa = np.arange(set_freqs)[:, None]
    lane = np.arange(LANES)[None, :]
    offset = block * (lane // half) + lane % half
    turn = 2.0 * np.pi / length
    angle = turn * (kappa * offset % length)
    base = np.stack([np.cos(angle), np.sin(angle)])
    which = np.arange(set_count)[:, None]
    angle = turn * (which * set_freqs * offset % length)
    phase = np.stack([np.cos(angle), np.sin(angle)], axis=1)
    phase = np.repeat(phase[:, :, None, :], 8, axis=2)
    period = length // (block * per_tile)
    angle = turn * (np.arange(period)[:, None] * block * per_tile % length)
    step = np.stack([np.cos(angle), np.sin(angle)])
    step = np.repeat(step, LANES, axis=2)
    rows = min(set_freqs, length // half)
    scale = 1.0 / math.sqrt(length * chan)
    angle = turn * (np.arange(rows)[:, None] * half % length)
    first = lane < chan
    merge = np.stack(
        [np.where(first, 1.0, np.cos(angle)) * scale, np.where(first, 0.0, np.sin(angle)) * scale]
    )
    index = np.arange(chan)
    angle = 2.0 * np.pi / chan * (index[:, None] * index[None, :] % chan)
    cos, sin, zero = np.cos(angle), np.sin(angle), np.zeros((chan, chan))
    mixer = np.block(
        [
            [cos, zero, zero, zero],
            [zero, cos, zero, -sin],
            [-sin, zero, zero, zero],
            [zero, -sin, zero, -cos],
        ]
    )
    f32 = [jnp.asarray(a, jnp.float32) for a in (base, phase, step, merge)]
    return f32 + [jnp.asarray(mixer, jnp.float32).astype(jnp.bfloat16)]


def kernel(
    row_count, col_count,
    tok_hbm, proj_hbm, gate_hbm, outw_hbm, base_hbm, phase_hbm, step_hbm, merge_hbm, mixer_hbm,
    out_ref,
    tok, proj, gate, outw, base, phase, step, merge, mixer,
    sendbuf, recv, tab, acc, pack, recv2,
    in_sem, send_sem, recv_sem, send2_sem, recv2_sem, own_sem,
):
    seq_count, block, width = tok.shape
    members = sendbuf.shape[0]
    half = block // 2
    chan = LANES // 2
    count = row_count * col_count
    row, col = lax.axis_index("row"), lax.axis_index("col")
    place = row * col_count + col
    order = col * row_count + row
    group_id, member = order // members, order % members

    def device(at):
        at = lax.rem(at, count)
        return (lax.rem(at, row_count), at // row_count)

    barrier = pltpu.get_barrier_semaphore()

    @pl.loop(1, count)
    def _(i):
        pl.semaphore_signal(barrier, inc=1, device_id=device(order + i), device_id_type=MESH)

    loads = [
        pltpu.make_async_copy(src, dst, in_sem.at[i])
        for i, (src, dst) in enumerate(
            [
                (tok_hbm, tok), (proj_hbm, proj), (gate_hbm, gate), (base_hbm, base),
                (phase_hbm.at[group_id], phase), (step_hbm, step), (merge_hbm, merge),
                (mixer_hbm, mixer), (outw_hbm, outw),
            ]
        )
    ]
    for load in loads:
        load.start()
    for load in loads[:3]:
        load.wait()

    flat = tok[...].reshape(seq_count * block, width)
    hidden = jnp.dot(flat, proj[...], preferred_element_type=jnp.float32)
    hidden = hidden.astype(jnp.bfloat16).astype(jnp.float32)
    gate_pre = jnp.dot(flat, gate[...], preferred_element_type=jnp.float32)
    mix = hidden * (gate_pre / (1.0 + jnp.exp(-gate_pre)))
    low = lax.broadcasted_iota(jnp.int32, (half, LANES), 1) < chan
    for s in range(seq_count):
        for t in range(GROUPS // 2):
            top = mix[s * block : s * block + half, t * LANES : (t + 1) * LANES]
            bottom = mix[s * block + half : (s + 1) * block, t * LANES : (t + 1) * LANES]
            even = jnp.where(low, top, pltpu.roll(bottom, chan, 1))
            odd = jnp.where(low, pltpu.roll(top, chan, 1), bottom)
            sendbuf[s * GROUPS + 2 * t] = even.astype(jnp.bfloat16)
            sendbuf[s * GROUPS + 2 * t + 1] = odd.astype(jnp.bfloat16)

    pl.semaphore_wait(barrier, count - 1)

    def copy_to(at):
        at = lax.rem(at, count)
        return pltpu.make_async_remote_copy(
            src_ref=sendbuf.at[lax.rem(at, members)],
            dst_ref=recv.at[place],
            send_sem=send_sem.at[at],
            recv_sem=recv_sem.at[place],
            device_id=device(at),
            device_id_type=MESH,
        )

    own = pltpu.make_async_copy(sendbuf.at[member], recv.at[place], own_sem)

    @pl.loop(1, count)
    def _(i):
        copy_to(order + lax.rem(i + count // 2 - 1, count - 1) + 1).start()

    own.start()

    for load in loads[3:]:
        load.wait()
    base_cos, base_sin = base[0], base[1]
    set_freqs = base_cos.shape[0]
    lane_cos, lane_sin = phase[0][:1], phase[1][:1]
    turned_cos = base_cos * lane_cos - base_sin * lane_sin
    turned_sin = base_sin * lane_cos + base_cos * lane_sin
    base[0], base[1] = turned_cos, turned_sin
    chunks, _, depth = tab.shape
    per_chunk = depth // LANES
    period = step.shape[1]
    step_cos, step_sin = step[0], step[1]

    def fill(c, now):
        for t in range(per_chunk):
            now_cos, now_sin = now
            bc = base[0].reshape(set_freqs // period, period, LANES)
            bs = base[1].reshape(set_freqs // period, period, LANES)
            tc = (bc * now_cos[None] - bs * now_sin[None]).reshape(set_freqs, LANES)
            ts = (bs * now_cos[None] + bc * now_sin[None]).reshape(set_freqs, LANES)
            tab[c, :set_freqs, t * LANES : (t + 1) * LANES] = tc.astype(jnp.bfloat16)
            tab[c, set_freqs:, t * LANES : (t + 1) * LANES] = ts.astype(jnp.bfloat16)
            now = (
                now_cos * step_cos - now_sin * step_sin,
                now_sin * step_cos + now_cos * step_sin,
            )
        return now

    start = (jnp.ones_like(step_cos), jnp.zeros_like(step_sin))
    lax.fori_loop(0, chunks, fill, start)

    own.wait()

    @pl.loop(1, count)
    def _(i):
        source = lax.rem(place + i, count)
        pltpu.make_async_remote_copy(
            src_ref=sendbuf.at[0],
            dst_ref=recv.at[source],
            send_sem=send_sem.at[0],
            recv_sem=recv_sem.at[source],
            device_id=(row, col),
            device_id_type=MESH,
        ).wait_recv()

    sources = depth // half

    def part(c):
        data = recv[pl.ds(c * sources, sources)].reshape(depth, LANES)
        return jnp.dot(tab[c], data, preferred_element_type=jnp.float32)

    if chunks == 1:
        total = part(0)
    else:
        acc[...] = part(0)

        @pl.loop(1, chunks)
        def _(c):
            acc[...] += part(c)

        total = acc[...]
    both = jnp.concatenate([total[:set_freqs], total[set_freqs:]], axis=1).astype(jnp.bfloat16)
    mixed = jnp.dot(both, mixer[...], preferred_element_type=jnp.float32)
    rows = merge.shape[1]
    kept = mixed[:, :LANES].reshape(set_freqs // rows, rows, LANES) * merge[0][None]
    kept = kept + mixed[:, LANES:].reshape(set_freqs // rows, rows, LANES) * merge[1][None]
    kept = kept.reshape(set_freqs, LANES)
    kept = kept + pltpu.roll(kept, chan, 1)
    for b in range(members):
        top = kept[b * block : b * block + half]
        bottom = kept[b * block + half : (b + 1) * block]
        pack[b] = jnp.where(low, top, bottom).astype(jnp.bfloat16)

    def back_to(b):
        return pltpu.make_async_remote_copy(
            src_ref=pack.at[b],
            dst_ref=recv2.at[member],
            send_sem=send2_sem.at[b],
            recv_sem=recv2_sem.at[member],
            device_id=device(group_id * members + b),
            device_id_type=MESH,
        )

    @pl.loop(1, members)
    def _(i):
        back_to(lax.rem(member + i, members)).start()

    own2 = pltpu.make_async_copy(pack.at[member], recv2.at[member], own_sem)
    own2.start()

    @pl.loop(1, count)
    def _(i):
        copy_to(order + i).wait_send()

    own2.wait()

    @pl.loop(1, members)
    def _(i):
        source = lax.rem(member + i, members)
        pltpu.make_async_remote_copy(
            src_ref=pack.at[0],
            dst_ref=recv2.at[source],
            send_sem=send2_sem.at[0],
            recv_sem=recv2_sem.at[source],
            device_id=(row, col),
            device_id_type=MESH,
        ).wait_recv()

    for s in range(seq_count):
        tops, bottoms = [], []
        for t in range(GROUPS // 2):
            even = recv2[s * GROUPS + 2 * t].astype(jnp.float32)
            odd = recv2[s * GROUPS + 2 * t + 1].astype(jnp.float32)
            tops.append(jnp.where(low, even, pltpu.roll(odd, chan, 1)))
            bottoms.append(jnp.where(low, pltpu.roll(even, chan, 1), odd))
        lhs = jnp.concatenate(
            [jnp.concatenate(tops, axis=1), jnp.concatenate(bottoms, axis=1)], axis=0
        ).astype(jnp.bfloat16)
        out_ref[s] = jnp.dot(lhs, outw[...], preferred_element_type=jnp.float32).astype(
            jnp.bfloat16
        )

    @pl.loop(1, members)
    def _(i):
        back_to(lax.rem(member + i, members)).wait_send()


def body(row_count, col_count, tokens, proj_weight, gate_weight, out_weight):
    seq_count, block, width = tokens.shape
    mixer_width = proj_weight.shape[1]
    chan = mixer_width // GROUPS
    members = seq_count * GROUPS
    count = row_count * col_count
    length = count * block
    set_count = count // members
    set_freqs = members * block
    half = block // 2
    consts = tables(length, set_count, block, seq_count, chan)
    base, phase, step, merge, mixer = consts
    depth = min(1024, count * half)
    chunks = count * half // depth
    bf16, f32 = jnp.bfloat16, jnp.float32
    dma = pltpu.SemaphoreType.DMA
    return pl.pallas_call(
        functools.partial(kernel, row_count, col_count),
        out_shape=jax.ShapeDtypeStruct((seq_count, block, out_weight.shape[1]), bf16),
        in_specs=[pl.BlockSpec(memory_space=pl.ANY)] * 9,
        out_specs=pl.BlockSpec(memory_space=pltpu.VMEM),
        scratch_shapes=[
            pltpu.VMEM(tokens.shape, bf16),
            pltpu.VMEM(proj_weight.shape, bf16),
            pltpu.VMEM(gate_weight.shape, bf16),
            pltpu.VMEM(out_weight.shape, bf16),
            pltpu.VMEM(base.shape, f32),
            pltpu.VMEM(phase.shape[1:], f32),
            pltpu.VMEM(step.shape, f32),
            pltpu.VMEM(merge.shape, f32),
            pltpu.VMEM(mixer.shape, bf16),
            pltpu.VMEM((members, half, LANES), bf16),
            pltpu.VMEM((count, half, LANES), bf16),
            pltpu.VMEM((chunks, 2 * set_freqs, depth), bf16),
            pltpu.VMEM((2 * set_freqs, LANES), f32),
            pltpu.VMEM((members, half, LANES), bf16),
            pltpu.VMEM((members, half, LANES), bf16),
            dma((9,)),
            dma((count,)),
            dma((count,)),
            dma((members,)),
            dma((members,)),
            dma,
        ],
        compiler_params=pltpu.CompilerParams(
            collective_id=0, has_side_effects=True, vmem_limit_bytes=56 * 1024 * 1024
        ),
    )(tokens, proj_weight, gate_weight, out_weight, *consts)


def solution(mesh):
    in_specs = (P(None, ("row", "col"), None), P(), P(), P())
    out_specs = P(None, ("col", "row"), None)
    run = functools.partial(body, mesh.shape["row"], mesh.shape["col"])
    return jax.shard_map(run, mesh=mesh, in_specs=in_specs, out_specs=out_specs, check_vma=False)
```

```python
import functools
import math

import jax
import jax.numpy as jnp
import numpy as np
from jax import lax
from jax.experimental import pallas as pl
from jax.experimental.pallas import tpu as pltpu
from jax.sharding import PartitionSpec as P

GROUPS = 4
LANES = 128
MESH = pl.DeviceIdType.MESH


def tables(length, set_count, block, seq_count, chan):
    set_freqs = length // set_count
    half = block // 2
    per_tile = LANES // half
    kappa = np.arange(set_freqs)[:, None]
    lane = np.arange(LANES)[None, :]
    offset = block * (lane // half) + lane % half
    turn = 2.0 * np.pi / length
    angle = turn * (kappa * offset % length)
    base = np.stack([np.cos(angle), np.sin(angle)])
    which = np.arange(set_count)[:, None]
    angle = turn * (which * set_freqs * offset % length)
    phase = np.stack([np.cos(angle), np.sin(angle)], axis=1)
    phase = np.repeat(phase[:, :, None, :], 8, axis=2)
    period = length // (block * per_tile)
    angle = turn * (np.arange(period)[:, None] * block * per_tile % length)
    step = np.stack([np.cos(angle), np.sin(angle)])
    step = np.repeat(step, LANES, axis=2)
    rows = min(set_freqs, length // half)
    scale = 1.0 / math.sqrt(length * chan)
    angle = turn * (np.arange(rows)[:, None] * half % length)
    first = lane < chan
    merge = np.stack(
        [np.where(first, 1.0, np.cos(angle)) * scale, np.where(first, 0.0, np.sin(angle)) * scale]
    )
    index = np.arange(chan)
    angle = 2.0 * np.pi / chan * (index[:, None] * index[None, :] % chan)
    cos, sin, zero = np.cos(angle), np.sin(angle), np.zeros((chan, chan))
    mixer = np.block(
        [
            [cos, zero, zero, zero],
            [zero, cos, zero, -sin],
            [-sin, zero, zero, zero],
            [zero, -sin, zero, -cos],
        ]
    )
    f32 = [jnp.asarray(a, jnp.float32) for a in (base, phase, step, merge)]
    return f32 + [jnp.asarray(mixer, jnp.float32).astype(jnp.bfloat16)]


def kernel(
    row_count, col_count,
    tok_hbm, proj_hbm, gate_hbm, base_hbm, phase_hbm, step_hbm, merge_hbm, mixer_hbm,
    out_ref,
    tok, proj, gate, base, phase, step, merge, mixer,
    sendbuf, recv, tab, acc, pack, recv2,
    in_sem, send_sem, recv_sem, send2_sem, recv2_sem, own_sem,
):
    seq_count, block, width = tok.shape
    members = sendbuf.shape[0]
    half = block // 2
    chan = LANES // 2
    count = row_count * col_count
    row, col = lax.axis_index("row"), lax.axis_index("col")
    place = row * col_count + col
    order = col * row_count + row
    group_id, member = order // members, order % members

    def device(at):
        at = lax.rem(at, count)
        return (lax.rem(at, row_count), at // row_count)

    barrier = pltpu.get_barrier_semaphore()

    @pl.loop(1, count)
    def _(i):
        pl.semaphore_signal(barrier, inc=1, device_id=device(order + i), device_id_type=MESH)

    loads = [
        pltpu.make_async_copy(src, dst, in_sem.at[i])
        for i, (src, dst) in enumerate(
            [
                (tok_hbm, tok), (proj_hbm, proj), (gate_hbm, gate), (base_hbm, base),
                (phase_hbm.at[group_id], phase), (step_hbm, step), (merge_hbm, merge),
                (mixer_hbm, mixer),
            ]
        )
    ]
    for load in loads:
        load.start()
    for load in loads[:3]:
        load.wait()

    flat = tok[...].reshape(seq_count * block, width)
    hidden = jnp.dot(flat, proj[...], preferred_element_type=jnp.float32)
    hidden = hidden.astype(jnp.bfloat16).astype(jnp.float32)
    gate_pre = jnp.dot(flat, gate[...], preferred_element_type=jnp.float32)
    mix = hidden * (gate_pre / (1.0 + jnp.exp(-gate_pre)))
    low = lax.broadcasted_iota(jnp.int32, (half, LANES), 1) < chan
    for s in range(seq_count):
        for t in range(GROUPS // 2):
            top = mix[s * block : s * block + half, t * LANES : (t + 1) * LANES]
            bottom = mix[s * block + half : (s + 1) * block, t * LANES : (t + 1) * LANES]
            even = jnp.where(low, top, pltpu.roll(bottom, chan, 1))
            odd = jnp.where(low, pltpu.roll(top, chan, 1), bottom)
            sendbuf[s * GROUPS + 2 * t] = even.astype(jnp.bfloat16)
            sendbuf[s * GROUPS + 2 * t + 1] = odd.astype(jnp.bfloat16)

    pl.semaphore_wait(barrier, count - 1)

    def copy_to(at):
        at = lax.rem(at, count)
        return pltpu.make_async_remote_copy(
            src_ref=sendbuf.at[lax.rem(at, members)],
            dst_ref=recv.at[place],
            send_sem=send_sem.at[at],
            recv_sem=recv_sem.at[place],
            device_id=device(at),
            device_id_type=MESH,
        )

    own = pltpu.make_async_copy(sendbuf.at[member], recv.at[place], own_sem)

    @pl.loop(1, count)
    def _(i):
        copy_to(order + i).start()

    own.start()

    for load in loads[3:]:
        load.wait()
    base_cos, base_sin = base[0], base[1]
    set_freqs = base_cos.shape[0]
    lane_cos, lane_sin = phase[0][:1], phase[1][:1]
    turned_cos = base_cos * lane_cos - base_sin * lane_sin
    turned_sin = base_sin * lane_cos + base_cos * lane_sin
    base[0], base[1] = turned_cos, turned_sin
    chunks, _, depth = tab.shape
    per_chunk = depth // LANES
    period = step.shape[1]
    step_cos, step_sin = step[0], step[1]

    def fill(c, now):
        for t in range(per_chunk):
            now_cos, now_sin = now
            bc = base[0].reshape(set_freqs // period, period, LANES)
            bs = base[1].reshape(set_freqs // period, period, LANES)
            tc = (bc * now_cos[None] - bs * now_sin[None]).reshape(set_freqs, LANES)
            ts = (bs * now_cos[None] + bc * now_sin[None]).reshape(set_freqs, LANES)
            tab[c, :set_freqs, t * LANES : (t + 1) * LANES] = tc.astype(jnp.bfloat16)
            tab[c, set_freqs:, t * LANES : (t + 1) * LANES] = ts.astype(jnp.bfloat16)
            now = (
                now_cos * step_cos - now_sin * step_sin,
                now_sin * step_cos + now_cos * step_sin,
            )
        return now

    start = (jnp.ones_like(step_cos), jnp.zeros_like(step_sin))
    lax.fori_loop(0, chunks, fill, start)


    own.wait()

    @pl.loop(1, count)
    def _(i):
        source = lax.rem(place + i, count)
        pltpu.make_async_remote_copy(
            src_ref=sendbuf.at[0],
            dst_ref=recv.at[source],
            send_sem=send_sem.at[0],
            recv_sem=recv_sem.at[source],
            device_id=(row, col),
            device_id_type=MESH,
        ).wait_recv()

    sources = depth // half

    def part(c):
        data = recv[pl.ds(c * sources, sources)].reshape(depth, LANES)
        return jnp.dot(tab[c], data, preferred_element_type=jnp.float32)

    if chunks == 1:
        total = part(0)
    else:
        acc[...] = part(0)

        @pl.loop(1, chunks)
        def _(c):
            acc[...] += part(c)

        total = acc[...]
    both = jnp.concatenate([total[:set_freqs], total[set_freqs:]], axis=1).astype(jnp.bfloat16)
    mixed = jnp.dot(both, mixer[...], preferred_element_type=jnp.float32)
    rows = merge.shape[1]
    kept = mixed[:, :LANES].reshape(set_freqs // rows, rows, LANES) * merge[0][None]
    kept = kept + mixed[:, LANES:].reshape(set_freqs // rows, rows, LANES) * merge[1][None]
    kept = kept.reshape(set_freqs, LANES)
    kept = kept + pltpu.roll(kept, chan, 1)
    for b in range(members):
        top = kept[b * block : b * block + half]
        bottom = kept[b * block + half : (b + 1) * block]
        pack[b] = jnp.where(low, top, bottom).astype(jnp.bfloat16)

    def back_to(b):
        return pltpu.make_async_remote_copy(
            src_ref=pack.at[b],
            dst_ref=recv2.at[member],
            send_sem=send2_sem.at[b],
            recv_sem=recv2_sem.at[member],
            device_id=device(group_id * members + b),
            device_id_type=MESH,
        )

    @pl.loop(1, members)
    def _(i):
        back_to(lax.rem(member + i, members)).start()

    own2 = pltpu.make_async_copy(pack.at[member], recv2.at[member], own_sem)
    own2.start()

    @pl.loop(1, count)
    def _(i):
        copy_to(order + i).wait_send()

    own2.wait()

    @pl.loop(1, members)
    def _(i):
        source = lax.rem(member + i, members)
        pltpu.make_async_remote_copy(
            src_ref=pack.at[0],
            dst_ref=recv2.at[source],
            send_sem=send2_sem.at[0],
            recv_sem=recv2_sem.at[source],
            device_id=(row, col),
            device_id_type=MESH,
        ).wait_recv()

    for s in range(seq_count):
        tops, bottoms = [], []
        for t in range(GROUPS // 2):
            even = recv2[s * GROUPS + 2 * t].astype(jnp.float32)
            odd = recv2[s * GROUPS + 2 * t + 1].astype(jnp.float32)
            tops.append(jnp.where(low, even, pltpu.roll(odd, chan, 1)))
            bottoms.append(jnp.where(low, pltpu.roll(even, chan, 1), odd))
        lhs = jnp.concatenate(
            [jnp.concatenate(tops, axis=1), jnp.concatenate(bottoms, axis=1)], axis=0
        ).astype(jnp.bfloat16)
        out_ref[s] = lhs

    @pl.loop(1, members)
    def _(i):
        back_to(lax.rem(member + i, members)).wait_send()


def body(row_count, col_count, tokens, proj_weight, gate_weight, out_weight):
    seq_count, block, width = tokens.shape
    mixer_width = proj_weight.shape[1]
    chan = mixer_width // GROUPS
    members = seq_count * GROUPS
    count = row_count * col_count
    length = count * block
    set_count = count // members
    set_freqs = members * block
    half = block // 2
    consts = tables(length, set_count, block, seq_count, chan)
    base, phase, step, merge, mixer = consts
    depth = min(1024, count * half)
    chunks = count * half // depth
    bf16, f32 = jnp.bfloat16, jnp.float32
    dma = pltpu.SemaphoreType.DMA
    mixed = pl.pallas_call(
        functools.partial(kernel, row_count, col_count),
        out_shape=jax.ShapeDtypeStruct((seq_count, block, mixer_width), bf16),
        in_specs=[pl.BlockSpec(memory_space=pl.ANY)] * 8,
        out_specs=pl.BlockSpec(memory_space=pltpu.VMEM),
        scratch_shapes=[
            pltpu.VMEM(tokens.shape, bf16),
            pltpu.VMEM(proj_weight.shape, bf16),
            pltpu.VMEM(gate_weight.shape, bf16),
            pltpu.VMEM(base.shape, f32),
            pltpu.VMEM(phase.shape[1:], f32),
            pltpu.VMEM(step.shape, f32),
            pltpu.VMEM(merge.shape, f32),
            pltpu.VMEM(mixer.shape, bf16),
            pltpu.VMEM((members, half, LANES), bf16),
            pltpu.VMEM((count, half, LANES), bf16),
            pltpu.VMEM((chunks, 2 * set_freqs, depth), bf16),
            pltpu.VMEM((2 * set_freqs, LANES), f32),
            pltpu.VMEM((members, half, LANES), bf16),
            pltpu.VMEM((members, half, LANES), bf16),
            dma((8,)),
            dma((count,)),
            dma((count,)),
            dma((members,)),
            dma((members,)),
            dma,
        ],
        compiler_params=pltpu.CompilerParams(
            collective_id=0, has_side_effects=True, vmem_limit_bytes=60 * 1024 * 1024
        ),
    )(tokens, proj_weight, gate_weight, *consts)
    result = jnp.einsum("stc,cd->std", mixed, out_weight, preferred_element_type=jnp.float32)
    return result.astype(bf16)


def solution(mesh):
    in_specs = (P(None, ("row", "col"), None), P(), P(), P())
    out_specs = P(None, ("col", "row"), None)
    run = functools.partial(body, mesh.shape["row"], mesh.shape["col"])
    return jax.shard_map(run, mesh=mesh, in_specs=in_specs, out_specs=out_specs, check_vma=False)
```

```python
import functools
import math

import jax
import jax.numpy as jnp
import numpy as np
from jax import lax
from jax.experimental import pallas as pl
from jax.experimental.pallas import tpu as pltpu
from jax.sharding import PartitionSpec as P

GROUPS = 4
LANES = 128
MESH = pl.DeviceIdType.MESH


def tables(length, set_count, block, seq_count, chan):
    set_freqs = length // set_count
    half = block // 2
    per_tile = LANES // half
    kappa = np.arange(set_freqs)[:, None]
    lane = np.arange(LANES)[None, :]
    offset = block * (lane // half) + lane % half
    turn = 2.0 * np.pi / length
    angle = turn * (kappa * offset % length)
    base = np.stack([np.cos(angle), np.sin(angle)])
    which = np.arange(set_count)[:, None]
    angle = turn * (which * set_freqs * offset % length)
    phase = np.stack([np.cos(angle), np.sin(angle)], axis=1)
    phase = np.repeat(phase[:, :, None, :], 8, axis=2)
    period = length // (block * per_tile)
    angle = turn * (np.arange(period)[:, None] * block * per_tile % length)
    step = np.stack([np.cos(angle), np.sin(angle)])
    step = np.repeat(step, LANES, axis=2)
    rows = min(set_freqs, length // half)
    scale = 1.0 / math.sqrt(length * chan)
    angle = turn * (np.arange(rows)[:, None] * half % length)
    first = lane < chan
    merge = np.stack(
        [np.where(first, 1.0, np.cos(angle)) * scale, np.where(first, 0.0, np.sin(angle)) * scale]
    )
    index = np.arange(chan)
    angle = 2.0 * np.pi / chan * (index[:, None] * index[None, :] % chan)
    cos, sin, zero = np.cos(angle), np.sin(angle), np.zeros((chan, chan))
    mixer = np.block(
        [
            [cos, zero, zero, zero],
            [zero, cos, zero, -sin],
            [-sin, zero, zero, zero],
            [zero, -sin, zero, -cos],
        ]
    )
    mixer = np.concatenate([mixer[:, :LANES], mixer[:, LANES:]])
    parts = [a.reshape(-1, LANES) for a in (base, step, merge, mixer, phase)]
    return jnp.asarray(np.concatenate(parts), jnp.float32), period, rows


def kernel(
    row_count, col_count, period, rows,
    tok_hbm, proj_hbm, gate_hbm, table_hbm,
    out_ref,
    tok, proj, gate, table,
    sendbuf, recv, tab, acc, pack, recv2,
    in_sem, send_sem, recv_sem, send2_sem, recv2_sem, own_sem,
):
    seq_count, block, width = tok.shape
    members = sendbuf.shape[0]
    half = block // 2
    chan = LANES // 2
    count = row_count * col_count
    row, col = lax.axis_index("row"), lax.axis_index("col")
    place = row * col_count + col
    order = col * row_count + row
    group_id, member = order // members, order % members

    def device(at):
        at = lax.rem(at, count)
        return (lax.rem(at, row_count), at // row_count)

    barrier = pltpu.get_barrier_semaphore()

    @pl.loop(1, count)
    def _(i):
        pl.semaphore_signal(barrier, inc=1, device_id=device(order + i), device_id_type=MESH)

    loads = [
        pltpu.make_async_copy(src, dst, in_sem.at[i])
        for i, (src, dst) in enumerate(
            [
                (tok_hbm, tok), (proj_hbm, proj), (gate_hbm, gate), (table_hbm, table),
            ]
        )
    ]
    for load in loads:
        load.start()
    for load in loads[:3]:
        load.wait()

    flat = tok[...].reshape(seq_count * block, width)
    hidden = jnp.dot(flat, proj[...], preferred_element_type=jnp.float32)
    hidden = hidden.astype(jnp.bfloat16).astype(jnp.float32)
    gate_pre = jnp.dot(flat, gate[...], preferred_element_type=jnp.float32)
    mix = hidden * (gate_pre / (1.0 + jnp.exp(-gate_pre)))
    low = lax.broadcasted_iota(jnp.int32, (half, LANES), 1) < chan
    for s in range(seq_count):
        for t in range(GROUPS // 2):
            top = mix[s * block : s * block + half, t * LANES : (t + 1) * LANES]
            bottom = mix[s * block + half : (s + 1) * block, t * LANES : (t + 1) * LANES]
            even = jnp.where(low, top, pltpu.roll(bottom, chan, 1))
            odd = jnp.where(low, pltpu.roll(top, chan, 1), bottom)
            sendbuf[s * GROUPS + 2 * t] = even.astype(jnp.bfloat16)
            sendbuf[s * GROUPS + 2 * t + 1] = odd.astype(jnp.bfloat16)

    pl.semaphore_wait(barrier, count - 1)

    def copy_to(at):
        at = lax.rem(at, count)
        return pltpu.make_async_remote_copy(
            src_ref=sendbuf.at[lax.rem(at, members)],
            dst_ref=recv.at[place],
            send_sem=send_sem.at[at],
            recv_sem=recv_sem.at[place],
            device_id=device(at),
            device_id_type=MESH,
        )

    own = pltpu.make_async_copy(sendbuf.at[member], recv.at[place], own_sem)

    @pl.loop(1, count)
    def _(i):
        copy_to(order + lax.rem(i + 2, count - 1) + 1).start()

    own.start()

    for load in loads[3:]:
        load.wait()
    chunks, set_freqs, depth = tab.shape
    set_freqs = set_freqs // 2
    base_cos, base_sin = table[:set_freqs], table[set_freqs : 2 * set_freqs]
    step_at = 2 * set_freqs
    merge_at = step_at + 2 * period
    mixer_at = merge_at + 2 * rows
    phase_at = mixer_at + 4 * LANES
    lane_cos = table[pl.ds(phase_at + group_id * 16, 8)][:1]
    lane_sin = table[pl.ds(phase_at + group_id * 16 + 8, 8)][:1]
    turned_cos = base_cos * lane_cos - base_sin * lane_sin
    turned_sin = base_sin * lane_cos + base_cos * lane_sin
    table[:set_freqs] = turned_cos
    table[set_freqs : 2 * set_freqs] = turned_sin
    per_chunk = depth // LANES
    step_cos = table[step_at : step_at + period]
    step_sin = table[step_at + period : merge_at]

    def fill(c, now):
        for t in range(per_chunk):
            now_cos, now_sin = now
            bc = table[:set_freqs].reshape(set_freqs // period, period, LANES)
            bs = table[set_freqs : 2 * set_freqs].reshape(set_freqs // period, period, LANES)
            tc = (bc * now_cos[None] - bs * now_sin[None]).reshape(set_freqs, LANES)
            ts = (bs * now_cos[None] + bc * now_sin[None]).reshape(set_freqs, LANES)
            tab[c, :set_freqs, t * LANES : (t + 1) * LANES] = tc.astype(jnp.bfloat16)
            tab[c, set_freqs:, t * LANES : (t + 1) * LANES] = ts.astype(jnp.bfloat16)
            now = (
                now_cos * step_cos - now_sin * step_sin,
                now_sin * step_cos + now_cos * step_sin,
            )
        return now

    start = (jnp.ones_like(step_cos), jnp.zeros_like(step_sin))
    lax.fori_loop(0, chunks, fill, start)


    own.wait()

    @pl.loop(1, count)
    def _(i):
        source = lax.rem(place + i, count)
        pltpu.make_async_remote_copy(
            src_ref=sendbuf.at[0],
            dst_ref=recv.at[source],
            send_sem=send_sem.at[0],
            recv_sem=recv_sem.at[source],
            device_id=(row, col),
            device_id_type=MESH,
        ).wait_recv()

    sources = depth // half

    def part(c):
        data = recv[pl.ds(c * sources, sources)].reshape(depth, LANES)
        return jnp.dot(tab[c], data, preferred_element_type=jnp.float32)

    if chunks == 1:
        total = part(0)
    else:
        acc[...] = part(0)

        @pl.loop(1, chunks)
        def _(c):
            acc[...] += part(c)

        total = acc[...]
    both = jnp.concatenate([total[:set_freqs], total[set_freqs:]], axis=1).astype(jnp.bfloat16)
    mixer = [table[mixer_at + 2 * LANES * i : mixer_at + 2 * LANES * (i + 1)] for i in (0, 1)]
    mixer = jnp.concatenate(mixer, axis=1).astype(jnp.bfloat16)
    mixed = jnp.dot(both, mixer, preferred_element_type=jnp.float32)
    keep, turn = table[merge_at : merge_at + rows], table[merge_at + rows : mixer_at]
    kept = mixed[:, :LANES].reshape(set_freqs // rows, rows, LANES) * keep[None]
    kept = kept + mixed[:, LANES:].reshape(set_freqs // rows, rows, LANES) * turn[None]
    kept = kept.reshape(set_freqs, LANES)
    kept = kept + pltpu.roll(kept, chan, 1)
    for b in range(members):
        top = kept[b * block : b * block + half]
        bottom = kept[b * block + half : (b + 1) * block]
        pack[b] = jnp.where(low, top, bottom).astype(jnp.bfloat16)

    def back_to(b):
        return pltpu.make_async_remote_copy(
            src_ref=pack.at[b],
            dst_ref=recv2.at[member],
            send_sem=send2_sem.at[b],
            recv_sem=recv2_sem.at[member],
            device_id=device(group_id * members + b),
            device_id_type=MESH,
        )

    @pl.loop(1, members)
    def _(i):
        back_to(lax.rem(member + i, members)).start()

    own2 = pltpu.make_async_copy(pack.at[member], recv2.at[member], own_sem)
    own2.start()

    @pl.loop(1, count)
    def _(i):
        copy_to(order + i).wait_send()

    own2.wait()

    @pl.loop(1, members)
    def _(i):
        source = lax.rem(member + i, members)
        pltpu.make_async_remote_copy(
            src_ref=pack.at[0],
            dst_ref=recv2.at[source],
            send_sem=send2_sem.at[0],
            recv_sem=recv2_sem.at[source],
            device_id=(row, col),
            device_id_type=MESH,
        ).wait_recv()

    for s in range(seq_count):
        tops, bottoms = [], []
        for t in range(GROUPS // 2):
            even = recv2[s * GROUPS + 2 * t].astype(jnp.float32)
            odd = recv2[s * GROUPS + 2 * t + 1].astype(jnp.float32)
            tops.append(jnp.where(low, even, pltpu.roll(odd, chan, 1)))
            bottoms.append(jnp.where(low, pltpu.roll(even, chan, 1), odd))
        lhs = jnp.concatenate(
            [jnp.concatenate(tops, axis=1), jnp.concatenate(bottoms, axis=1)], axis=0
        ).astype(jnp.bfloat16)
        out_ref[s] = lhs

    @pl.loop(1, members)
    def _(i):
        back_to(lax.rem(member + i, members)).wait_send()


def body(row_count, col_count, tokens, proj_weight, gate_weight, out_weight):
    seq_count, block, width = tokens.shape
    mixer_width = proj_weight.shape[1]
    chan = mixer_width // GROUPS
    members = seq_count * GROUPS
    count = row_count * col_count
    length = count * block
    set_count = count // members
    set_freqs = members * block
    half = block // 2
    table, period, rows = tables(length, set_count, block, seq_count, chan)
    depth = min(1024, count * half)
    chunks = count * half // depth
    bf16, f32 = jnp.bfloat16, jnp.float32
    dma = pltpu.SemaphoreType.DMA
    mixed = pl.pallas_call(
        functools.partial(kernel, row_count, col_count, period, rows),
        out_shape=jax.ShapeDtypeStruct((seq_count, block, mixer_width), bf16),
        in_specs=[pl.BlockSpec(memory_space=pl.ANY)] * 4,
        out_specs=pl.BlockSpec(memory_space=pltpu.VMEM),
        scratch_shapes=[
            pltpu.VMEM(tokens.shape, bf16),
            pltpu.VMEM(proj_weight.shape, bf16),
            pltpu.VMEM(gate_weight.shape, bf16),
            pltpu.VMEM(table.shape, f32),
            pltpu.VMEM((members, half, LANES), bf16),
            pltpu.VMEM((count, half, LANES), bf16),
            pltpu.VMEM((chunks, 2 * set_freqs, depth), bf16),
            pltpu.VMEM((2 * set_freqs, LANES), f32),
            pltpu.VMEM((members, half, LANES), bf16),
            pltpu.VMEM((members, half, LANES), bf16),
            dma((4,)),
            dma((count,)),
            dma((count,)),
            dma((members,)),
            dma((members,)),
            dma,
        ],
        compiler_params=pltpu.CompilerParams(
            collective_id=0, has_side_effects=True, vmem_limit_bytes=56360960
        ),
    )(tokens, proj_weight, gate_weight, table)
    result = jnp.einsum("stc,cd->std", mixed, out_weight, preferred_element_type=jnp.float32)
    return result.astype(bf16)


def solution(mesh):
    in_specs = (P(None, ("row", "col"), None), P(), P(), P())
    out_specs = P(None, ("col", "row"), None)
    run = functools.partial(body, mesh.shape["row"], mesh.shape["col"])
    return jax.shard_map(run, mesh=mesh, in_specs=in_specs, out_specs=out_specs, check_vma=False)
```

```python
import functools
import math

import jax
import jax.numpy as jnp
import numpy as np
from jax import lax
from jax.experimental import pallas as pl
from jax.experimental.pallas import tpu as pltpu
from jax.sharding import PartitionSpec as P

GROUPS = 4
LANES = 128
MESH = pl.DeviceIdType.MESH


def tables(length, set_count, block, seq_count, chan):
    set_freqs = length // set_count
    half = block // 2
    per_tile = LANES // half
    kappa = np.arange(set_freqs)[:, None]
    lane = np.arange(LANES)[None, :]
    offset = block * (lane // half) + lane % half
    turn = 2.0 * np.pi / length
    angle = turn * (kappa * offset % length)
    base = np.stack([np.cos(angle), np.sin(angle)])
    which = np.arange(set_count)[:, None]
    angle = turn * (which * set_freqs * offset % length)
    phase = np.stack([np.cos(angle), np.sin(angle)], axis=1)
    phase = np.repeat(phase[:, :, None, :], 8, axis=2)
    period = length // (block * per_tile)
    angle = turn * (np.arange(period)[:, None] * block * per_tile % length)
    step = np.stack([np.cos(angle), np.sin(angle)])
    step = np.repeat(step, LANES, axis=2)
    rows = min(set_freqs, length // half)
    scale = 1.0 / math.sqrt(length * chan)
    angle = turn * (np.arange(rows)[:, None] * half % length)
    first = lane < chan
    merge = np.stack(
        [np.where(first, 1.0, np.cos(angle)) * scale, np.where(first, 0.0, np.sin(angle)) * scale]
    )
    index = np.arange(chan)
    angle = 2.0 * np.pi / chan * (index[:, None] * index[None, :] % chan)
    cos, sin, zero = np.cos(angle), np.sin(angle), np.zeros((chan, chan))
    mixer = np.block(
        [
            [cos, zero, zero, zero],
            [zero, cos, zero, -sin],
            [-sin, zero, zero, zero],
            [zero, -sin, zero, -cos],
        ]
    )
    mixer = np.concatenate([mixer[:, :LANES], mixer[:, LANES:]])
    parts = [a.reshape(-1, LANES) for a in (base, step, merge, mixer, phase)]
    return jnp.asarray(np.concatenate(parts), jnp.float32), period, rows


def kernel(
    row_count, col_count, period, rows,
    tok_hbm, proj_hbm, gate_hbm, table_hbm,
    out_ref,
    tok, proj, gate, table,
    sendbuf, recv, tab, acc, pack, recv2,
    in_sem, send_sem, recv_sem, send2_sem, recv2_sem, own_sem,
):
    seq_count, block, width = tok.shape
    members = sendbuf.shape[0]
    half = block // 2
    chan = LANES // 2
    count = row_count * col_count
    row, col = lax.axis_index("row"), lax.axis_index("col")
    place = row * col_count + col
    order = col * row_count + row
    group_id, member = order // members, order % members

    def device(at):
        at = lax.rem(at, count)
        return (lax.rem(at, row_count), at // row_count)

    barrier = pltpu.get_barrier_semaphore()

    @pl.loop(1, count)
    def _(i):
        pl.semaphore_signal(barrier, inc=1, device_id=device(order + i), device_id_type=MESH)

    loads = [
        pltpu.make_async_copy(src, dst, in_sem.at[i])
        for i, (src, dst) in enumerate(
            [
                (tok_hbm, tok), (proj_hbm, proj), (gate_hbm, gate), (table_hbm, table),
            ]
        )
    ]
    for load in loads:
        load.start()
    for load in loads[:3]:
        load.wait()

    flat = tok[...].reshape(seq_count * block, width)
    hidden = jnp.dot(flat, proj[...], preferred_element_type=jnp.float32)
    hidden = hidden.astype(jnp.bfloat16).astype(jnp.float32)
    gate_pre = jnp.dot(flat, gate[...], preferred_element_type=jnp.float32)
    mix = hidden * (gate_pre / (1.0 + jnp.exp(-gate_pre)))
    low = lax.broadcasted_iota(jnp.int32, (half, LANES), 1) < chan
    for s in range(seq_count):
        for t in range(GROUPS // 2):
            top = mix[s * block : s * block + half, t * LANES : (t + 1) * LANES]
            bottom = mix[s * block + half : (s + 1) * block, t * LANES : (t + 1) * LANES]
            even = jnp.where(low, top, pltpu.roll(bottom, chan, 1))
            odd = jnp.where(low, pltpu.roll(top, chan, 1), bottom)
            sendbuf[s * GROUPS + 2 * t] = even.astype(jnp.bfloat16)
            sendbuf[s * GROUPS + 2 * t + 1] = odd.astype(jnp.bfloat16)

    pl.semaphore_wait(barrier, count - 1)

    def copy_to(at):
        at = lax.rem(at, count)
        return pltpu.make_async_remote_copy(
            src_ref=sendbuf.at[lax.rem(at, members)],
            dst_ref=recv.at[place],
            send_sem=send_sem.at[at],
            recv_sem=recv_sem.at[place],
            device_id=device(at),
            device_id_type=MESH,
        )

    own = pltpu.make_async_copy(sendbuf.at[member], recv.at[place], own_sem)

    @pl.loop(1, count)
    def _(i):
        copy_to(order + lax.rem(i + 2, count - 1) + 1).start()

    own.start()

    for load in loads[3:]:
        load.wait()
    chunks, set_freqs, depth = tab.shape
    set_freqs = set_freqs // 2
    base_cos, base_sin = table[:set_freqs], table[set_freqs : 2 * set_freqs]
    step_at = 2 * set_freqs
    merge_at = step_at + 2 * period
    mixer_at = merge_at + 2 * rows
    phase_at = mixer_at + 4 * LANES
    lane_cos = table[pl.ds(phase_at + group_id * 16, 8)][:1]
    lane_sin = table[pl.ds(phase_at + group_id * 16 + 8, 8)][:1]
    turned_cos = base_cos * lane_cos - base_sin * lane_sin
    turned_sin = base_sin * lane_cos + base_cos * lane_sin
    table[:set_freqs] = turned_cos
    table[set_freqs : 2 * set_freqs] = turned_sin
    per_chunk = depth // LANES
    step_cos = table[step_at : step_at + period]
    step_sin = table[step_at + period : merge_at]

    def fill(c, now):
        for t in range(per_chunk):
            now_cos, now_sin = now
            bc = table[:set_freqs].reshape(set_freqs // period, period, LANES)
            bs = table[set_freqs : 2 * set_freqs].reshape(set_freqs // period, period, LANES)
            tc = (bc * now_cos[None] - bs * now_sin[None]).reshape(set_freqs, LANES)
            ts = (bs * now_cos[None] + bc * now_sin[None]).reshape(set_freqs, LANES)
            tab[c, :set_freqs, t * LANES : (t + 1) * LANES] = tc.astype(jnp.bfloat16)
            tab[c, set_freqs:, t * LANES : (t + 1) * LANES] = ts.astype(jnp.bfloat16)
            now = (
                now_cos * step_cos - now_sin * step_sin,
                now_sin * step_cos + now_cos * step_sin,
            )
        return now

    start = (jnp.ones_like(step_cos), jnp.zeros_like(step_sin))
    lax.fori_loop(0, chunks, fill, start)


    own.wait()

    @pl.loop(1, count)
    def _(i):
        source = lax.rem(place + i, count)
        pltpu.make_async_remote_copy(
            src_ref=sendbuf.at[0],
            dst_ref=recv.at[source],
            send_sem=send_sem.at[0],
            recv_sem=recv_sem.at[source],
            device_id=(row, col),
            device_id_type=MESH,
        ).wait_recv()

    sources = depth // half

    def part(c):
        data = recv[pl.ds(c * sources, sources)].reshape(depth, LANES)
        return jnp.dot(tab[c], data, preferred_element_type=jnp.float32)

    if chunks == 1:
        total = part(0)
    else:
        acc[...] = part(0)

        @pl.loop(1, chunks)
        def _(c):
            acc[...] += part(c)

        total = acc[...]
    both = jnp.concatenate([total[:set_freqs], total[set_freqs:]], axis=1).astype(jnp.bfloat16)
    mixer = [table[mixer_at + 2 * LANES * i : mixer_at + 2 * LANES * (i + 1)] for i in (0, 1)]
    mixer = jnp.concatenate(mixer, axis=1).astype(jnp.bfloat16)
    mixed = jnp.dot(both, mixer, preferred_element_type=jnp.float32)
    keep, turn = table[merge_at : merge_at + rows], table[merge_at + rows : mixer_at]
    kept = mixed[:, :LANES].reshape(set_freqs // rows, rows, LANES) * keep[None]
    kept = kept + mixed[:, LANES:].reshape(set_freqs // rows, rows, LANES) * turn[None]
    kept = kept.reshape(set_freqs, LANES)
    kept = kept + pltpu.roll(kept, chan, 1)
    def back_to(b):
        return pltpu.make_async_remote_copy(
            src_ref=pack.at[b],
            dst_ref=recv2.at[member],
            send_sem=send2_sem.at[b],
            recv_sem=recv2_sem.at[member],
            device_id=device(group_id * members + b),
            device_id_type=MESH,
        )

    for b in range(members):
        top = kept[b * block : b * block + half]
        bottom = kept[b * block + half : (b + 1) * block]
        pack[b] = jnp.where(low, top, bottom).astype(jnp.bfloat16)

        @pl.when(b != member)
        def _():
            back_to(b).start()

    own2 = pltpu.make_async_copy(pack.at[member], recv2.at[member], own_sem)
    own2.start()

    @pl.loop(1, count)
    def _(i):
        copy_to(order + i).wait_send()

    own2.wait()

    @pl.loop(1, members)
    def _(i):
        source = lax.rem(member + i, members)
        pltpu.make_async_remote_copy(
            src_ref=pack.at[0],
            dst_ref=recv2.at[source],
            send_sem=send2_sem.at[0],
            recv_sem=recv2_sem.at[source],
            device_id=(row, col),
            device_id_type=MESH,
        ).wait_recv()

    for s in range(seq_count):
        tops, bottoms = [], []
        for t in range(GROUPS // 2):
            even = recv2[s * GROUPS + 2 * t].astype(jnp.float32)
            odd = recv2[s * GROUPS + 2 * t + 1].astype(jnp.float32)
            tops.append(jnp.where(low, even, pltpu.roll(odd, chan, 1)))
            bottoms.append(jnp.where(low, pltpu.roll(even, chan, 1), odd))
        lhs = jnp.concatenate(
            [jnp.concatenate(tops, axis=1), jnp.concatenate(bottoms, axis=1)], axis=0
        ).astype(jnp.bfloat16)
        out_ref[s] = lhs

    @pl.loop(1, members)
    def _(i):
        back_to(lax.rem(member + i, members)).wait_send()


def body(row_count, col_count, tokens, proj_weight, gate_weight, out_weight):
    seq_count, block, width = tokens.shape
    mixer_width = proj_weight.shape[1]
    chan = mixer_width // GROUPS
    members = seq_count * GROUPS
    count = row_count * col_count
    length = count * block
    set_count = count // members
    set_freqs = members * block
    half = block // 2
    table, period, rows = tables(length, set_count, block, seq_count, chan)
    depth = min(1024, count * half)
    chunks = count * half // depth
    bf16, f32 = jnp.bfloat16, jnp.float32
    dma = pltpu.SemaphoreType.DMA
    mixed = pl.pallas_call(
        functools.partial(kernel, row_count, col_count, period, rows),
        out_shape=jax.ShapeDtypeStruct((seq_count, block, mixer_width), bf16),
        in_specs=[pl.BlockSpec(memory_space=pl.ANY)] * 4,
        out_specs=pl.BlockSpec(memory_space=pltpu.VMEM),
        scratch_shapes=[
            pltpu.VMEM(tokens.shape, bf16),
            pltpu.VMEM(proj_weight.shape, bf16),
            pltpu.VMEM(gate_weight.shape, bf16),
            pltpu.VMEM(table.shape, f32),
            pltpu.VMEM((members, half, LANES), bf16),
            pltpu.VMEM((count, half, LANES), bf16),
            pltpu.VMEM((chunks, 2 * set_freqs, depth), bf16),
            pltpu.VMEM((2 * set_freqs, LANES), f32),
            pltpu.VMEM((members, half, LANES), bf16),
            pltpu.VMEM((members, half, LANES), bf16),
            dma((4,)),
            dma((count,)),
            dma((count,)),
            dma((members,)),
            dma((members,)),
            dma,
        ],
        compiler_params=pltpu.CompilerParams(
            collective_id=0, has_side_effects=True, vmem_limit_bytes=56360960
        ),
    )(tokens, proj_weight, gate_weight, table)
    result = jnp.einsum("stc,cd->std", mixed, out_weight, preferred_element_type=jnp.float32)
    return result.astype(bf16)


def solution(mesh):
    in_specs = (P(None, ("row", "col"), None), P(), P(), P())
    out_specs = P(None, ("col", "row"), None)
    run = functools.partial(body, mesh.shape["row"], mesh.shape["col"])
    return jax.shard_map(run, mesh=mesh, in_specs=in_specs, out_specs=out_specs, check_vma=False)
```
